32 devices in a mesh: sp: 8 (over z, core), tp: 4 (over y, x).
Axes of the slice: x: 2, y: 2, z: 4, core: 2. Of those that a mesh axis runs over, the one named last changes fastest.
Arguments:
- prompt: bfloat16 [8, 2048, 2048], P('tp', 'sp'), may hold values from -6 to 6
- input_gain: float32 [2048], replicated, may hold values from 0.1 to 1.9
- key_weight: bfloat16 [1024, 2048], P('tp'), may hold values from -0.125 to 0.125
- value_weight: bfloat16 [1024, 2048], P('tp'), may hold values from -0.125 to 0.125
- key_gain: float32 [64], replicated, may hold values from 0.1 to 1.9
- queries: bfloat16 [8, 2, 1024], P('sp', None, 'tp'), may hold values from -6 to 6
- score_bias: float32 [2, 16], replicated, may hold values from -9 to -2
Outputs:
- keys: bfloat16 [8, 1024, 2048], P('sp', 'tp')
- values: bfloat16 [8, 1024, 2048], P('sp', 'tp')
- first_read: bfloat16 [8, 2, 1024], P('sp', None, 'tp')
The draws below stay inside these ranges and needn't reach their ends.
All inputs are finite; a program needn't handle non-finite values.
Results may differ from the reference program's by a relative error of at most 0.01.
Values may be sent and summed in bfloat16 or wider, within the bound.
No kernel may reach another device: no remote copies, remote signals or barrier semaphores. Data moves between devices by JAX's collectives and lax.ppermute only.
A program may use at most 64 MiB of HBM per device.

```python
import math
import jax
import jax.numpy as jnp
from jax import lax

D = 2048
KV_HEADS = 16
HEAD = 64
GROUP = 2
SEQS = 8
LEN = 2048
KVW = 1024


def shard_levels(key, extent, split, low, high):
    def one(position, blocks):
        draws = jax.random.uniform(jax.random.fold_in(jax.random.fold_in(key, 6), position), (blocks,), jnp.float32, low / len(split), high / len(split))
        return jnp.repeat(jnp.exp(draws), extent[position] // blocks).reshape((-1,) + (1,) * (len(extent) - position - 1))

    loudness = one(*split[0])
    for cut in split[1:]:
        loudness = loudness * one(*cut)
    return loudness


def gaussian(stream_key, dims, scale, reach, shards=(), held_as=jnp.bfloat16):
    array = jax.random.normal(stream_key, dims, jnp.float32) * scale
    if len(shards) > 0:
        array = shard_levels(stream_key, dims, shards, -0.22, 0.18) * array
    return jnp.clip(array, min=-reach, max=reach).astype(held_as)


def setup_inputs(seed: int = 0) -> dict:
    key_of = jax.random.split(jax.random.key(seed), 8)
    prompt = gaussian(key_of[0], (SEQS, LEN, D), 1.0, 6.0, ((0, 4), (1, 8)))
    input_gain = jnp.clip(1.0 + 0.18 * jax.random.normal(key_of[1], (D,), jnp.float32), 0.1, 1.9)
    key_weight = gaussian(key_of[2], (KVW, D), D ** -0.5, 0.125, ((0, 4),))
    value_weight = gaussian(key_of[3], (KVW, D), D ** -0.5, 0.125, ((0, 4),))
    key_gain = jnp.clip(1.0 + 0.18 * jax.random.normal(key_of[4], (HEAD,), jnp.float32), 0.1, 1.9)
    queries = gaussian(key_of[5], (SEQS, GROUP, KVW), 1.0, 6.0, ((0, 8), (2, 4)))
    score_bias = jnp.clip(jax.random.uniform(key_of[6], (GROUP, KV_HEADS), jnp.float32, -9.0, -2.0), -9.0, -2.0)
    return dict(prompt=prompt, input_gain=input_gain, key_weight=key_weight, value_weight=value_weight, key_gain=key_gain, queries=queries, score_bias=score_bias)


epsilon = 1e-06

def reference(prompt, input_gain, key_weight, value_weight, key_gain, queries, score_bias):

    def one_sequence(pair):
        rows, query = pair
        flat = rows.astype(jnp.float32)
        normed = (flat * lax.rsqrt(lax.optimization_barrier(jnp.mean(flat * flat, axis=-1, keepdims=True)) + epsilon) * input_gain).astype(jnp.bfloat16)
        key_raw = jnp.dot(normed, key_weight.T, preferred_element_type=jnp.float32).reshape(LEN, KV_HEADS, HEAD)
        key_norm = (key_raw * lax.rsqrt(lax.optimization_barrier(jnp.mean(key_raw * key_raw, axis=-1, keepdims=True)) + epsilon) * key_gain).astype(jnp.bfloat16)
        value_rows = jnp.dot(normed, value_weight.T, preferred_element_type=jnp.float32).astype(jnp.bfloat16)
        query_heads = query.astype(jnp.float32).reshape(GROUP, KV_HEADS, HEAD)
        scores = jnp.einsum('ghd,shd->ghs', query_heads, key_norm.astype(jnp.float32)) / math.sqrt(HEAD)
        scores = scores + score_bias[:, :, None]
        log_break = jax.nn.log_sigmoid(scores)
        log_keep = jax.nn.log_sigmoid(-scores)
        later = lax.cumsum(log_keep, axis=2, reverse=True) - log_keep
        weights = jnp.exp(log_break + later).astype(jnp.bfloat16)
        value_heads = value_rows.astype(jnp.float32).reshape(LEN, KV_HEADS, HEAD)
        read = jnp.einsum('ghs,shd->ghd', weights.astype(jnp.float32), value_heads).astype(jnp.bfloat16)
        return (key_norm.reshape(LEN, KVW).T, value_rows.T, read.reshape(GROUP, KVW))
    keys, values, first_read = lax.map(one_sequence, (prompt, queries))
    return (keys, values, first_read)
```

```python
import functools
import math

import jax
import jax.numpy as jnp
from jax import lax
from jax.experimental import pallas as pl
from jax.experimental.pallas import tpu as pltpu
from jax.sharding import PartitionSpec as P

HEAD = 64
CORES = 2
CHUNKS = 2

epsilon = 1e-06


def project_kernel(place, gain, *refs, tp, seqs, relays):
    weights = refs[: len(relays)]
    own, other = refs[len(relays) : len(relays) + 2]
    outs = refs[len(relays) + 2 : -4]
    weight_buf, row_buf, weight_sems, row_sems = refs[-4:]
    core = place[0]
    columns = weight_buf.shape[1]
    copies = []
    for n, (ref, (block, start, size)) in enumerate(zip(weights, relays)):
        copies.append(
            pltpu.make_async_copy(
                ref, weight_buf.at[place[1 + block], pl.ds(start, size)], weight_sems.at[n]
            )
        )
    copies.append(pltpu.make_async_copy(own, row_buf.at[core], row_sems.at[0]))
    copies.append(pltpu.make_async_copy(other, row_buf.at[1 - core], row_sems.at[1]))
    for copy in copies:
        copy.start()
    for copy in copies:
        copy.wait()
    width = weight_buf.shape[2]
    stacked = weight_buf[...].reshape(tp * columns, width)
    is_key = core == 0
    for turn in range(seqs):
        seq = (core + turn) % seqs
        for half in range(CORES):
            raw = lax.dot_general(
                stacked,
                row_buf[half, seq],
                (((1,), (1,)), ((), ())),
                preferred_element_type=jnp.float32,
            )
            heads = raw.reshape(tp * columns // HEAD, HEAD, raw.shape[1])
            scale = lax.rsqrt(jnp.mean(heads * heads, axis=1, keepdims=True) + epsilon)
            factor = jnp.where(is_key, scale * gain[...][None], 1.0)
            done = (heads * factor).reshape(tp, columns, raw.shape[1]).astype(jnp.bfloat16)
            for hop in range(tp):
                outs[hop * seqs + turn][half] = done[hop]


def project(weights, relays, own, other, place, gain, tp):
    seqs, rows, width = own.shape
    columns = max(start + size for _, start, size in relays)
    block = jax.ShapeDtypeStruct((CORES, columns, rows), jnp.bfloat16)
    anywhere = pl.BlockSpec(memory_space=pl.ANY)
    return pl.pallas_call(
        functools.partial(project_kernel, tp=tp, seqs=seqs, relays=relays),
        out_shape=[block] * (tp * seqs),
        in_specs=[
            pl.BlockSpec(memory_space=pltpu.SMEM),
            pl.BlockSpec(memory_space=pltpu.VMEM),
        ]
        + [anywhere] * (len(weights) + 2),
        out_specs=[pl.BlockSpec(memory_space=pltpu.VMEM)] * (tp * seqs),
        scratch_shapes=[
            pltpu.VMEM((tp, columns, width), jnp.bfloat16),
            pltpu.VMEM((CORES, seqs, rows, width), jnp.bfloat16),
            pltpu.SemaphoreType.DMA((len(weights),)),
            pltpu.SemaphoreType.DMA((CORES,)),
        ],
        name="project",
    )(place, gain, *weights, own, other)


def read_kernel(place, query, bias, *refs, chunks, hops, turns):
    count = chunks * hops * turns
    pieces = refs[:count]
    keys, values, read = refs[count : count + 3]
    buf, sems, out_sems = refs[count + 3 :]
    core = place[0]
    columns, length = buf.shape[1:]
    rows = pieces[0].shape[2]
    step = columns // chunks
    copies = []
    for n, piece in enumerate(pieces):
        chunk, hop, turn = n // (hops * turns), n // turns % hops, n % turns
        for half in range(CORES):
            start = pl.multiple_of((place[1 + hop] * CORES + half) * rows, rows)
            target = buf.at[(core + turn) % CORES, pl.ds(chunk * step, step), pl.ds(start, rows)]
            copies.append(pltpu.make_async_copy(piece.at[half], target, sems.at[n, half]))
    for copy in copies:
        copy.start()
    for copy in copies:
        copy.wait()
    outs = [
        pltpu.make_async_copy(buf.at[0], keys, out_sems.at[0]),
        pltpu.make_async_copy(buf.at[1], values, out_sems.at[1]),
    ]
    for copy in outs:
        copy.start()
    group = query.shape[0]
    heads = columns // HEAD
    lanes = lax.broadcasted_iota(jnp.int32, (heads, columns), 1) // HEAD
    mine = lanes == lax.broadcasted_iota(jnp.int32, (heads, columns), 0)
    spread = jnp.concatenate(
        [jnp.where(mine, query[g : g + 1, :].astype(jnp.float32), 0.0) for g in range(group)], axis=0
    ).astype(jnp.bfloat16)
    scores = lax.dot_general(
        spread, buf[0], (((1,), (0,)), ((), ())), preferred_element_type=jnp.float32
    )
    scores = scores / math.sqrt(HEAD) + bias[...]
    keep = -(jnp.maximum(scores, 0.0) + jnp.log1p(jnp.exp(-jnp.abs(scores))))
    span = 128
    after = (
        lax.broadcasted_iota(jnp.int32, (span, span), 0)
        > lax.broadcasted_iota(jnp.int32, (span, span), 1)
    ).astype(jnp.float32)
    carry = jnp.zeros((group * heads, 1), jnp.float32)
    weights = []
    for n in reversed(range(length // span)):
        part = keep[:, n * span : (n + 1) * span]
        later = lax.dot_general(
            part,
            after,
            (((1,), (0,)), ((), ())),
            precision=lax.Precision.HIGHEST,
            preferred_element_type=jnp.float32,
        )
        total = scores[:, n * span : (n + 1) * span] + part + later + carry
        weights.append(jnp.exp(total).astype(jnp.bfloat16))
        carry = carry + jnp.sum(part, axis=1, keepdims=True)
    mixed = lax.dot_general(
        jnp.concatenate(weights[::-1], axis=1),
        buf[1],
        (((1,), (1,)), ((), ())),
        preferred_element_type=jnp.float32,
    )
    read[...] = jnp.concatenate(
        [
            jnp.sum(
                jnp.where(mine, mixed[g * heads : (g + 1) * heads], 0.0), axis=0, keepdims=True
            )
            for g in range(group)
        ],
        axis=0,
    ).astype(jnp.bfloat16)
    for copy in outs:
        copy.wait()


def read_cache(pieces, place, query, bias, chunks, hops, turns, columns, length):
    cache = jax.ShapeDtypeStruct((columns, length), jnp.bfloat16)
    anywhere = pl.BlockSpec(memory_space=pl.ANY)
    vmem = pl.BlockSpec(memory_space=pltpu.VMEM)
    return pl.pallas_call(
        functools.partial(read_kernel, chunks=chunks, hops=hops, turns=turns),
        out_shape=[cache, cache, jax.ShapeDtypeStruct(query.shape, jnp.bfloat16)],
        in_specs=[pl.BlockSpec(memory_space=pltpu.SMEM), vmem, vmem] + [anywhere] * len(pieces),
        out_specs=[anywhere, anywhere, vmem],
        scratch_shapes=[
            pltpu.VMEM((CORES, columns, length), jnp.bfloat16),
            pltpu.SemaphoreType.DMA((len(pieces), CORES)),
            pltpu.SemaphoreType.DMA((CORES,)),
        ],
        name="read_cache",
    )(place, query, bias, *pieces)


def local(prompt, input_gain, key_weight, value_weight, key_gain, queries, score_bias):
    sp, tp = lax.axis_size("sp"), lax.axis_size("tp")
    seqs = prompt.shape[0]
    chips = sp // CORES
    assert sp == seqs * tp and seqs == CORES
    place_sp, place_tp = lax.axis_index("sp"), lax.axis_index("tp")
    chip, core = place_sp // CORES, place_sp % CORES
    columns = key_weight.shape[0]
    heads_here = columns // HEAD
    chunks = math.gcd(CHUNKS, heads_here)
    step = columns // chunks
    side = math.isqrt(tp)

    def along_tp(array, hop):
        return lax.ppermute(array, "tp", [(n, n ^ hop) for n in range(tp)])

    weight = jnp.where(core == 0, key_weight, value_weight)
    gathered = []
    for chunk in range(chunks):
        part = weight[chunk * step : (chunk + 1) * step]
        if gathered:
            part = lax.optimization_barrier((part, gathered[-1][0][1:3]))[0]
        if side == 2:
            half = step // 2
            near = along_tp(part, 1)
            far = along_tp(part, side)
            relayed = along_tp(far[:half], 1)
            crossed = along_tp(near[half:], side)
            gathered.append(
                (
                    [part, near, far, relayed, crossed],
                    ((0, 0, step), (1, 0, step), (2, 0, step), (3, 0, half), (3, half, half)),
                )
            )
        else:
            gathered.append(
                (
                    [part] + [along_tp(part, hop) for hop in range(1, tp)],
                    tuple((hop, 0, step) for hop in range(tp)),
                )
            )

    flat = prompt.astype(jnp.float32)
    normed = (
        flat * lax.rsqrt(jnp.mean(flat * flat, axis=-1, keepdims=True) + epsilon) * input_gain
    ).astype(jnp.bfloat16)
    other = lax.ppermute(normed, "sp", [(n, n ^ 1) for n in range(sp)])

    hops = jnp.arange(tp, dtype=jnp.int32)
    slots = ((place_tp ^ hops) - chip) % tp
    send_place = jnp.concatenate([core[None], slots]).astype(jnp.int32)
    pieces = []
    for blocks, relays in gathered:
        outs = project(blocks, relays, normed, other, send_place, key_gain[:, None], tp)
        for hop in range(tp):
            for turn in range(seqs):
                pairs = []
                for s in range(sp):
                    for t in range(tp):
                        to_sp = seqs * t + (s % CORES + turn) % seqs
                        to_tp = (s // CORES + hop) % tp
                        pairs.append((s * tp + t, to_sp * tp + to_tp))
                pieces.append(lax.ppermute(outs[hop * seqs + turn], ("sp", "tp"), pairs))

    heads = lax.dynamic_slice_in_dim(score_bias, place_tp * heads_here, heads_here, 1)
    read_place = jnp.concatenate([core[None], (place_tp - hops) % chips]).astype(jnp.int32)
    keys, values, read = read_cache(
        pieces,
        read_place,
        queries[0],
        heads.reshape(-1, 1),
        chunks,
        tp,
        seqs,
        columns,
        prompt.shape[1] * sp,
    )
    return keys[None], values[None], read[None]


def solution(mesh):
    placed = (P("tp", "sp", None), P(), P("tp", None), P("tp", None), P(), P("sp", None, "tp"), P())
    return jax.shard_map(
        local,
        mesh=mesh,
        in_specs=placed,
        out_specs=(P("sp", "tp", None), P("sp", "tp", None), P("sp", None, "tp")),
        check_vma=False,
    )
```

```python
import functools
import math

import jax
import jax.numpy as jnp
from jax import lax
from jax.experimental import pallas as pl
from jax.experimental.pallas import tpu as pltpu
from jax.sharding import PartitionSpec as P


HEAD = 64
CORES = 2
CHUNKS = 2

epsilon = 1e-06


def project_kernel(place, gain, *refs, tp, seqs, relays):
    weights = refs[: len(relays)]
    own, other = refs[len(relays) : len(relays) + 2]
    outs = refs[len(relays) + 2 : -4]
    weight_buf, row_buf, weight_sems, row_sems = refs[-4:]
    core = place[0]
    columns, width = weight_buf.shape[1:]
    copies = [
        pltpu.make_async_copy(own, row_buf.at[0], row_sems.at[0]),
        pltpu.make_async_copy(other, row_buf.at[1], row_sems.at[1]),
    ]
    loads = [
        pltpu.make_async_copy(
            ref, weight_buf.at[block, pl.ds(start, size)], weight_sems.at[n]
        )
        for n, (ref, (block, start, size)) in enumerate(zip(weights, relays))
    ]
    for copy in loads + copies:
        copy.start()
    for copy in loads:
        copy.wait()
    stacked = weight_buf[...].reshape(tp * columns, width)
    is_key = core == 0
    for half in range(CORES):
        copies[half].wait()
        for seq in range(seqs):
            raw = lax.dot_general(
                stacked,
                row_buf[half, seq],
                (((1,), (1,)), ((), ())),
                preferred_element_type=jnp.float32,
            )
            heads = raw.reshape(tp * columns // HEAD, HEAD, raw.shape[1])
            scale = lax.rsqrt(jnp.mean(heads * heads, axis=1, keepdims=True) + epsilon)
            factor = jnp.where(is_key, scale * gain[...][None], 1.0)
            done = (heads * factor).reshape(tp, columns, raw.shape[1]).astype(jnp.bfloat16)
            for hop in range(tp):
                outs[hop][seq, (core + half) % CORES] = done[hop]


def project(weights, relays, own, other, place, gain, tp):
    seqs, rows, width = own.shape
    columns = max(start + size for _, start, size in relays)
    anywhere = pl.BlockSpec(memory_space=pl.ANY)
    return pl.pallas_call(
        functools.partial(project_kernel, tp=tp, seqs=seqs, relays=relays),
        out_shape=[jax.ShapeDtypeStruct((seqs, CORES, columns, rows), jnp.bfloat16)] * tp,
        in_specs=[
            pl.BlockSpec(memory_space=pltpu.SMEM),
            pl.BlockSpec(memory_space=pltpu.VMEM),
        ]
        + [anywhere] * (len(weights) + 2),
        out_specs=[pl.BlockSpec(memory_space=pltpu.VMEM)] * tp,
        scratch_shapes=[
            pltpu.VMEM((tp, columns, width), jnp.bfloat16),
            pltpu.VMEM((CORES, seqs, rows, width), jnp.bfloat16),
            pltpu.SemaphoreType.DMA((len(weights),)),
            pltpu.SemaphoreType.DMA((CORES,)),
        ],
        name="project",
    )(place, gain, *weights, own, other)


def order_kernel(place, *refs):
    blocks, out, sems = refs[:-2], refs[-2], refs[-1]
    copies = [
        pltpu.make_async_copy(block, out.at[place[1 + n]], sems.at[n]) for n, block in enumerate(blocks)
    ]
    for copy in copies:
        copy.start()
    for copy in copies:
        copy.wait()


def order(blocks, place):
    anywhere = pl.BlockSpec(memory_space=pl.ANY)
    return pl.pallas_call(
        order_kernel,
        out_shape=jax.ShapeDtypeStruct((len(blocks),) + blocks[0].shape, blocks[0].dtype),
        in_specs=[pl.BlockSpec(memory_space=pltpu.SMEM)] + [anywhere] * len(blocks),
        out_specs=anywhere,
        scratch_shapes=[pltpu.SemaphoreType.DMA((len(blocks),))],
        name="order",
    )(place, *blocks)


def read_kernel(query, bias, *refs):
    pieces = refs[:-6]
    keys, values, read, buf, sems, out_sems = refs[-6:]
    columns = buf.shape[1]
    rows = pieces[0].shape[3]
    step = columns // len(pieces)
    copies = []
    for chunk, piece in enumerate(pieces):
        for source in range(piece.shape[0]):
            for half in range(CORES):
                start = (source // CORES * CORES + half) * rows
                target = buf.at[
                    source % CORES, chunk * step : (chunk + 1) * step, start : start + rows
                ]
                copies.append(
                    pltpu.make_async_copy(
                        piece.at[source, half], target, sems.at[chunk, source, half]
                    )
                )
    for copy in copies:
        copy.start()
    for copy in copies:
        copy.wait()
    outs = [
        pltpu.make_async_copy(buf.at[0], keys, out_sems.at[0]),
        pltpu.make_async_copy(buf.at[1], values, out_sems.at[1]),
    ]
    for copy in outs:
        copy.start()
    length = buf.shape[2]
    group = query.shape[0]
    heads = columns // HEAD
    lanes = lax.broadcasted_iota(jnp.int32, (heads, columns), 1) // HEAD
    mine = lanes == lax.broadcasted_iota(jnp.int32, (heads, columns), 0)
    spread = jnp.concatenate(
        [jnp.where(mine, query[g : g + 1, :].astype(jnp.float32), 0.0) for g in range(group)], axis=0
    ).astype(jnp.bfloat16)
    scores = lax.dot_general(
        spread, buf[0], (((1,), (0,)), ((), ())), preferred_element_type=jnp.float32
    )
    scores = scores / math.sqrt(HEAD) + bias[...]
    keep = -(jnp.maximum(scores, 0.0) + jnp.log1p(jnp.exp(-jnp.abs(scores))))
    span = 128
    after = (
        lax.broadcasted_iota(jnp.int32, (span, span), 0)
        > lax.broadcasted_iota(jnp.int32, (span, span), 1)
    ).astype(jnp.float32)
    carry = jnp.zeros((group * heads, 1), jnp.float32)
    weights = []
    for n in reversed(range(length // span)):
        part = keep[:, n * span : (n + 1) * span]
        later = lax.dot_general(
            part,
            after,
            (((1,), (0,)), ((), ())),
            precision=lax.Precision.HIGHEST,
            preferred_element_type=jnp.float32,
        )
        total = scores[:, n * span : (n + 1) * span] + part + later + carry
        weights.append(jnp.exp(total).astype(jnp.bfloat16))
        carry = carry + jnp.sum(part, axis=1, keepdims=True)
    mixed = lax.dot_general(
        jnp.concatenate(weights[::-1], axis=1),
        buf[1],
        (((1,), (1,)), ((), ())),
        preferred_element_type=jnp.float32,
    )
    read[...] = jnp.concatenate(
        [
            jnp.sum(
                jnp.where(mine, mixed[g * heads : (g + 1) * heads], 0.0), axis=0, keepdims=True
            )
            for g in range(group)
        ],
        axis=0,
    ).astype(jnp.bfloat16)
    for copy in outs:
        copy.wait()


def read_cache(pieces, query, bias, columns, length):
    cache = jax.ShapeDtypeStruct((columns, length), jnp.bfloat16)
    anywhere = pl.BlockSpec(memory_space=pl.ANY)
    vmem = pl.BlockSpec(memory_space=pltpu.VMEM)
    return pl.pallas_call(
        read_kernel,
        out_shape=[cache, cache, jax.ShapeDtypeStruct(query.shape, jnp.bfloat16)],
        in_specs=[vmem, vmem] + [anywhere] * len(pieces),
        out_specs=[anywhere, anywhere, vmem],
        scratch_shapes=[
            pltpu.VMEM((CORES, columns, length), jnp.bfloat16),
            pltpu.SemaphoreType.DMA((len(pieces), pieces[0].shape[0], CORES)),
            pltpu.SemaphoreType.DMA((CORES,)),
        ],
        name="read_cache",
    )(query, bias, *pieces)


def body(prompt, input_gain, key_weight, value_weight, key_gain, queries, score_bias):
    sp, tp = lax.axis_size("sp"), lax.axis_size("tp")
    seqs = prompt.shape[0]
    assert sp == seqs * tp and seqs == CORES
    place_sp, place_tp = lax.axis_index("sp"), lax.axis_index("tp")
    core = place_sp % CORES
    columns = key_weight.shape[0]
    heads_here = columns // HEAD
    chunks = math.gcd(CHUNKS, heads_here)
    step = columns // chunks
    side = math.isqrt(tp)

    def along_tp(array, hop):
        return lax.ppermute(array, "tp", [(n, n ^ hop) for n in range(tp)])

    weight = jnp.where(core == 0, key_weight, value_weight)
    gathered = []
    for chunk in range(chunks):
        part = weight[chunk * step : (chunk + 1) * step]
        if side == 2:
            half = step // 2
            low, high = part[:half], part[half:]
            if gathered:
                low, high, _ = lax.optimization_barrier((low, high, gathered[-1][0][2:6]))
            near_high = along_tp(high, 1)
            far_low = along_tp(low, side)
            near_low = along_tp(low, 1)
            far_high = along_tp(high, side)
            relayed = along_tp(far_low, 1)
            crossed = along_tp(near_high, side)
            blocks = [low, high, near_low, near_high, far_low, far_high, relayed, crossed]
            gathered.append((blocks, tuple((n // 2, n % 2 * half, half) for n in range(2 * tp))))
        else:
            gathered.append(
                (
                    [part] + [along_tp(part, hop) for hop in range(1, tp)],
                    tuple((hop, 0, step) for hop in range(tp)),
                )
            )

    flat = prompt.astype(jnp.float32)
    normed = (
        flat * lax.rsqrt(jnp.mean(flat * flat, axis=-1, keepdims=True) + epsilon) * input_gain
    ).astype(jnp.bfloat16)
    other = lax.ppermute(normed, "sp", [(n, n ^ 1) for n in range(sp)])

    peers = place_tp ^ jnp.arange(tp, dtype=jnp.int32)
    place = jnp.concatenate([core[None], peers]).astype(jnp.int32)
    pieces = []
    ordered = ()
    for blocks, relays in gathered:
        low, own, _ = lax.optimization_barrier((blocks[0], normed, ordered))
        blocks = [low] + blocks[1:]
        outs = project(blocks, relays, own, other, place, key_gain[:, None], tp)
        ordered = order([outs[0]] + [along_tp(outs[hop], hop) for hop in range(1, tp)], place)
        by_sequence = ordered.reshape((sp,) + ordered.shape[2:])
        pieces.append(lax.all_to_all(by_sequence, "sp", split_axis=0, concat_axis=0, tiled=True))

    heads = lax.dynamic_slice_in_dim(score_bias, place_tp * heads_here, heads_here, 1)
    keys, values, read = read_cache(
        pieces, queries[0], heads.reshape(-1, 1), columns, prompt.shape[1] * sp
    )
    return keys[None], values[None], read[None]


def solution(mesh):
    placed = (P("tp", "sp", None), P(), P("tp", None), P("tp", None), P(), P("sp", None, "tp"), P())
    return jax.shard_map(
        body,
        mesh=mesh,
        in_specs=placed,
        out_specs=(P("sp", "tp", None), P("sp", "tp", None), P("sp", None, "tp")),
        check_vma=False,
    )
```

```python
import functools
import math

import jax
import jax.numpy as jnp
from jax import lax
from jax.experimental import pallas as pl
from jax.experimental.pallas import tpu as pltpu
from jax.sharding import PartitionSpec as P


HEAD = 64
CORES = 2
CHUNKS = 2

epsilon = 1e-06


def project_kernel(place, gain, *refs, tp, seqs, relays):
    weights = refs[: len(relays)]
    own, other = refs[len(relays) : len(relays) + 2]
    outs = refs[len(relays) + 2 : -4]
    weight_buf, row_buf, weight_sems, row_sems = refs[-4:]
    core = place[0]
    columns, width = weight_buf.shape[1:]
    copies = [
        pltpu.make_async_copy(own, row_buf.at[0], row_sems.at[0]),
        pltpu.make_async_copy(other, row_buf.at[1], row_sems.at[1]),
    ]
    loads = [
        pltpu.make_async_copy(
            ref, weight_buf.at[block, pl.ds(start, size)], weight_sems.at[n]
        )
        for n, (ref, (block, start, size)) in enumerate(zip(weights, relays))
    ]
    for copy in loads + copies:
        copy.start()
    for copy in loads:
        copy.wait()
    stacked = weight_buf[...].reshape(tp * columns, width)
    is_key = core == 0
    for half in range(CORES):
        copies[half].wait()
        for seq in range(seqs):
            raw = lax.dot_general(
                stacked,
                row_buf[half, seq],
                (((1,), (1,)), ((), ())),
                preferred_element_type=jnp.float32,
            )
            heads = raw.reshape(tp * columns // HEAD, HEAD, raw.shape[1])
            scale = lax.rsqrt(jnp.mean(heads * heads, axis=1, keepdims=True) + epsilon)
            factor = jnp.where(is_key, scale * gain[...][None], 1.0)
            done = (heads * factor).reshape(tp, columns, raw.shape[1]).astype(jnp.bfloat16)
            for hop in range(tp):
                outs[hop][seq, (core + half) % CORES] = done[hop]


def project(weights, relays, own, other, place, gain, tp):
    seqs, rows, width = own.shape
    columns = max(start + size for _, start, size in relays)
    anywhere = pl.BlockSpec(memory_space=pl.ANY)
    return pl.pallas_call(
        functools.partial(project_kernel, tp=tp, seqs=seqs, relays=relays),
        out_shape=[jax.ShapeDtypeStruct((seqs, CORES, columns, rows), jnp.bfloat16)] * tp,
        in_specs=[
            pl.BlockSpec(memory_space=pltpu.SMEM),
            pl.BlockSpec(memory_space=pltpu.VMEM),
        ]
        + [anywhere] * (len(weights) + 2),
        out_specs=[pl.BlockSpec(memory_space=pltpu.VMEM)] * tp,
        scratch_shapes=[
            pltpu.VMEM((tp, columns, width), jnp.bfloat16),
            pltpu.VMEM((CORES, seqs, rows, width), jnp.bfloat16),
            pltpu.SemaphoreType.DMA((len(weights),)),
            pltpu.SemaphoreType.DMA((CORES,)),
        ],
        name="project",
    )(place, gain, *weights, own, other)


def order_kernel(place, *refs):
    blocks, out, sems = refs[:-2], refs[-2], refs[-1]
    copies = [
        pltpu.make_async_copy(block, out.at[place[1 + n]], sems.at[n]) for n, block in enumerate(blocks)
    ]
    for copy in copies:
        copy.start()
    for copy in copies:
        copy.wait()


def order(blocks, place):
    anywhere = pl.BlockSpec(memory_space=pl.ANY)
    return pl.pallas_call(
        order_kernel,
        out_shape=jax.ShapeDtypeStruct((len(blocks),) + blocks[0].shape, blocks[0].dtype),
        in_specs=[pl.BlockSpec(memory_space=pltpu.SMEM)] + [anywhere] * len(blocks),
        out_specs=pl.BlockSpec(memory_space=pltpu.VMEM),
        scratch_shapes=[pltpu.SemaphoreType.DMA((len(blocks),))],
        name="order",
    )(place, *blocks)


def read_kernel(query, bias, *refs):
    pieces = refs[:-6]
    keys, values, read, buf, sems, out_sems = refs[-6:]
    columns = buf.shape[1]
    rows = pieces[0].shape[3]
    step = columns // len(pieces)
    copies = []
    for chunk, piece in enumerate(pieces):
        for source in range(piece.shape[0]):
            for half in range(CORES):
                start = (source // CORES * CORES + half) * rows
                target = buf.at[
                    source % CORES, chunk * step : (chunk + 1) * step, start : start + rows
                ]
                copies.append(
                    pltpu.make_async_copy(
                        piece.at[source, half], target, sems.at[chunk, source, half]
                    )
                )
    for copy in copies:
        copy.start()
    for copy in copies:
        copy.wait()
    outs = [
        pltpu.make_async_copy(buf.at[0], keys, out_sems.at[0]),
        pltpu.make_async_copy(buf.at[1], values, out_sems.at[1]),
    ]
    for copy in outs:
        copy.start()
    length = buf.shape[2]
    group = query.shape[0]
    heads = columns // HEAD
    lanes = lax.broadcasted_iota(jnp.int32, (heads, columns), 1) // HEAD
    mine = lanes == lax.broadcasted_iota(jnp.int32, (heads, columns), 0)
    spread = jnp.concatenate(
        [jnp.where(mine, query[g : g + 1, :].astype(jnp.float32), 0.0) for g in range(group)], axis=0
    ).astype(jnp.bfloat16)
    scores = lax.dot_general(
        spread, buf[0], (((1,), (0,)), ((), ())), preferred_element_type=jnp.float32
    )
    scores = scores / math.sqrt(HEAD) + bias[...]
    keep = -(jnp.maximum(scores, 0.0) + jnp.log1p(jnp.exp(-jnp.abs(scores))))
    span = 128
    after = (
        lax.broadcasted_iota(jnp.int32, (span, span), 0)
        > lax.broadcasted_iota(jnp.int32, (span, span), 1)
    ).astype(jnp.float32)
    carry = jnp.zeros((group * heads, 1), jnp.float32)
    weights = []
    for n in reversed(range(length // span)):
        part = keep[:, n * span : (n + 1) * span]
        later = lax.dot_general(
            part,
            after,
            (((1,), (0,)), ((), ())),
            precision=lax.Precision.HIGHEST,
            preferred_element_type=jnp.float32,
        )
        total = scores[:, n * span : (n + 1) * span] + part + later + carry
        weights.append(jnp.exp(total).astype(jnp.bfloat16))
        carry = carry + jnp.sum(part, axis=1, keepdims=True)
    mixed = lax.dot_general(
        jnp.concatenate(weights[::-1], axis=1),
        buf[1],
        (((1,), (1,)), ((), ())),
        preferred_element_type=jnp.float32,
    )
    read[...] = jnp.concatenate(
        [
            jnp.sum(
                jnp.where(mine, mixed[g * heads : (g + 1) * heads], 0.0), axis=0, keepdims=True
            )
            for g in range(group)
        ],
        axis=0,
    ).astype(jnp.bfloat16)
    for copy in outs:
        copy.wait()


def read_cache(pieces, query, bias, columns, length):
    cache = jax.ShapeDtypeStruct((columns, length), jnp.bfloat16)
    anywhere = pl.BlockSpec(memory_space=pl.ANY)
    vmem = pl.BlockSpec(memory_space=pltpu.VMEM)
    return pl.pallas_call(
        read_kernel,
        out_shape=[cache, cache, jax.ShapeDtypeStruct(query.shape, jnp.bfloat16)],
        in_specs=[vmem, vmem] + [anywhere] * len(pieces),
        out_specs=[anywhere, anywhere, vmem],
        scratch_shapes=[
            pltpu.VMEM((CORES, columns, length), jnp.bfloat16),
            pltpu.SemaphoreType.DMA((len(pieces), pieces[0].shape[0], CORES)),
            pltpu.SemaphoreType.DMA((CORES,)),
        ],
        name="read_cache",
    )(query, bias, *pieces)


def body(prompt, input_gain, key_weight, value_weight, key_gain, queries, score_bias):
    sp, tp = lax.axis_size("sp"), lax.axis_size("tp")
    seqs = prompt.shape[0]
    assert sp == seqs * tp and seqs == CORES
    place_sp, place_tp = lax.axis_index("sp"), lax.axis_index("tp")
    core = place_sp % CORES
    columns = key_weight.shape[0]
    heads_here = columns // HEAD
    chunks = math.gcd(CHUNKS, heads_here)
    step = columns // chunks
    side = math.isqrt(tp)

    def along_tp(array, hop):
        return lax.ppermute(array, "tp", [(n, n ^ hop) for n in range(tp)])

    weight = jnp.where(core == 0, key_weight, value_weight)
    weight, prompt = lax.optimization_barrier((weight, prompt))
    gathered = []
    for chunk in range(chunks):
        part = weight[chunk * step : (chunk + 1) * step]
        if side == 2:
            half = step // 2
            low, high = part[:half], part[half:]
            if gathered:
                low, high, _ = lax.optimization_barrier((low, high, gathered[-1][0][2:6]))
            near_high = along_tp(high, 1)
            far_low = along_tp(low, side)
            near_low = along_tp(low, 1)
            far_high = along_tp(high, side)
            relayed = along_tp(far_low, 1)
            crossed = along_tp(near_high, side)
            blocks = [low, high, near_low, near_high, far_low, far_high, relayed, crossed]
            gathered.append((blocks, tuple((n // 2, n % 2 * half, half) for n in range(2 * tp))))
        else:
            gathered.append(
                (
                    [part] + [along_tp(part, hop) for hop in range(1, tp)],
                    tuple((hop, 0, step) for hop in range(tp)),
                )
            )

    flat = prompt.astype(jnp.float32)
    normed = (
        flat * lax.rsqrt(jnp.mean(flat * flat, axis=-1, keepdims=True) + epsilon) * input_gain
    ).astype(jnp.bfloat16)
    other = lax.ppermute(normed, "sp", [(n, n ^ 1) for n in range(sp)])

    peers = place_tp ^ jnp.arange(tp, dtype=jnp.int32)
    place = jnp.concatenate([core[None], peers]).astype(jnp.int32)
    pieces = []
    ordered = ()
    for blocks, relays in gathered:
        low, own, _ = lax.optimization_barrier((blocks[0], normed, ordered))
        blocks = [low] + blocks[1:]
        outs = project(blocks, relays, own, other, place, key_gain[:, None], tp)
        sent = [outs[0]] + [along_tp(outs[hop], hop) for hop in range(1, tp)]
        ordered = order(sent, place)
        by_sequence = ordered.reshape((sp,) + ordered.shape[2:])
        pieces.append(lax.all_to_all(by_sequence, "sp", split_axis=0, concat_axis=0, tiled=True))

    heads = lax.dynamic_slice_in_dim(score_bias, place_tp * heads_here, heads_here, 1)
    keys, values, read = read_cache(
        pieces, queries[0], heads.reshape(-1, 1), columns, prompt.shape[1] * sp
    )
    return keys[None], values[None], read[None]


def solution(mesh):
    placed = (P("tp", "sp", None), P(), P("tp", None), P("tp", None), P(), P("sp", None, "tp"), P())
    return jax.shard_map(
        body,
        mesh=mesh,
        in_specs=placed,
        out_specs=(P("sp", "tp", None), P("sp", "tp", None), P("sp", None, "tp")),
        check_vma=False,
    )
```
